32 devices in a mesh: sp: 16 (over z, y, x), tp: 2 (over core).
Axes of the slice: x: 2, y: 2, z: 4, core: 2. Of those that a mesh axis runs over, the one named last changes fastest.
Arguments:
- conv_value: bfloat16 [8192, 1536], P('sp', 'tp'), may hold values from -6 to 6
- conv_gate: bfloat16 [8192, 1536], P('sp', 'tp'), may hold values from -8 to 8
- conv_out: bfloat16 [8192, 1536], P('sp', 'tp'), may hold values from -40 to 40
- conv_taps: bfloat16 [31, 1536], P(None, 'tp'), may hold values from -1 to 1
- norm_gain: float32 [1536], P('tp'), may hold values from 0.1 to 1.9
- norm_shift: float32 [1536], P('tp'), may hold values from -3 to 3
- proj_weight: bfloat16 [2048, 1536], P(None, 'tp'), may hold values from -0.15625 to 0.15625
- out_grad: bfloat16 [8192, 2048], P('sp'), may hold values from -6 to 6
Outputs:
- grad_value: bfloat16 [8192, 1536], P('sp', 'tp')
- grad_gate: bfloat16 [8192, 1536], P('sp', 'tp')
- grad_taps: float32 [31, 1536], P(None, 'tp')
- grad_gain: float32 [1536], P('tp')
- grad_shift: float32 [1536], P('tp')
- grad_proj: float32 [2048, 1536], P('sp', 'tp')
The draws below stay inside these ranges and needn't reach their ends.
All inputs are finite; a program needn't handle non-finite values.
Results may differ from the reference program's by a relative error of at most 0.005.
Values may be sent and summed in bfloat16 or wider, within the bound.
A program may use at most 64 MiB of HBM per device.

```python
import jax
import jax.numpy as jnp
from jax import lax

D = 2048
CH = 1536
TAPS = 31
SEQ = 8192


def draw_conv_out(key, part):
    key_scale, key_group, key_base, key_mean = jax.random.split(key, 4)
    chan_scale = jnp.exp(jax.random.uniform(key_scale, (CH,), jnp.float32, -1.0, 1.0))
    group_scale = jnp.exp(jax.random.uniform(key_group, (8,), jnp.float32, -1.2, 1.2))
    group_index = jnp.arange(CH) * 8 // CH
    scales = chan_scale * group_scale[group_index]
    base = jax.random.normal(key_base, (SEQ, CH), jnp.float32) * scales
    offset = jax.random.normal(key_mean, (SEQ, 1), jnp.float32)
    return jnp.clip(base + offset, -40.0, 40.0).astype(jnp.bfloat16)


def spiked(values, rng, source, target, parts, factor):
    def block_of(position):
        return (jnp.arange(values.shape[position]) // (values.shape[position] // parts)).reshape((-1,) + (1,) * (values.ndim - 1 - position))

    one_side = jax.random.permutation(rng, parts)[block_of(target)]
    other_side = (block_of(target) + parts // 2) % parts
    return jnp.where((block_of(source) == one_side) | (block_of(source) == other_side), factor * values, values)


def steps_of(stream_key, extent, shards, smallest, high):
    def one(axis_at, parts):
        steps = jax.random.uniform(jax.random.fold_in(jax.random.fold_in(stream_key, 6), axis_at), (parts,), jnp.float32, smallest / len(shards), high / len(shards))
        return jnp.repeat(jnp.exp(steps), extent[axis_at] // parts).reshape((-1,) + (1,) * (len(extent) - axis_at - 1))

    factor_of = one(*shards[0])
    for cut in shards[1:]:
        factor_of = factor_of * one(*cut)
    return factor_of


def bell_draw(own_key, dims, scale, limit, cuts=(), held_as=jnp.bfloat16):
    entries = jax.random.normal(own_key, dims, jnp.float32) * scale
    if len(cuts) > 0:
        entries = steps_of(own_key, dims, cuts, -0.22, 0.18) * entries
    return jnp.clip(entries, min=-limit, max=limit).astype(held_as)


def noise_with(key, extent, spread, reach, pieces, heavy, held_as=jnp.bfloat16):
    drawn = spread * jax.random.normal(key, extent, jnp.float32)
    if pieces:
        drawn = drawn * steps_of(key, extent, pieces, -0.22, 0.18)
    return jnp.clip(spiked(drawn, jax.random.fold_in(key, 3), *heavy), -reach, reach).astype(held_as)


def setup_inputs(seed: int = 0) -> dict:
    splits = jax.random.split(jax.random.key(seed), 9)
    return {
        "conv_value": bell_draw(splits[0], (SEQ, CH), 1.0, 6.0, ((0, 16), (1, 2))),
        "conv_gate": bell_draw(splits[1], (SEQ, CH), 1.5, 8.0, ((0, 16), (1, 2))),
        "conv_out": draw_conv_out(jax.random.fold_in(splits[8], 71), 0),
        "conv_taps": bell_draw(splits[3], (TAPS, CH), TAPS ** -0.5, 1.0, ((1, 2),)),
        "norm_gain": jnp.clip(1.0 + 0.18 * jax.random.normal(splits[4], (CH,), jnp.float32), 0.1, 1.9),
        "norm_shift": bell_draw(splits[5], (CH,), 0.5, 3.0, ((0, 2),), jnp.float32),
        "proj_weight": bell_draw(splits[6], (D, CH), CH ** -0.5, 0.15625, ((1, 2),)),
        "out_grad": noise_with(splits[7], (SEQ, D), 1.0, 6.0, ((0, 16),), (0, 1, 16, 2.0)),
    }


norm_eps = 1e-05

def reference(conv_value, conv_gate, conv_out, conv_taps, norm_gain, norm_shift, proj_weight, out_grad):
    height = conv_out.astype(jnp.float32)
    center = lax.optimization_barrier(jnp.mean(height, axis=1, keepdims=True))
    centered = height - center
    variance = lax.optimization_barrier(jnp.mean(centered * centered, axis=1, keepdims=True))
    inv_std = lax.rsqrt(variance + norm_eps)
    normed = centered * inv_std
    shifted = normed * norm_gain + norm_shift
    sig_norm = jax.nn.sigmoid(shifted)
    active = (shifted * sig_norm).astype(jnp.bfloat16)
    grad_proj = jnp.dot(out_grad.T, active, preferred_element_type=jnp.float32)
    act_grad = jnp.dot(out_grad, proj_weight, preferred_element_type=jnp.float32)
    norm_grad = act_grad * (sig_norm * (1.0 + shifted * (1.0 - sig_norm)))
    grad_gain = lax.optimization_barrier(jnp.sum(norm_grad * normed, axis=0))
    grad_shift = lax.optimization_barrier(jnp.sum(norm_grad, axis=0))
    scaled = norm_grad * norm_gain
    height_grad = inv_std * (scaled - lax.optimization_barrier(jnp.mean(scaled, axis=1, keepdims=True)) - normed * lax.optimization_barrier(jnp.mean(scaled * normed, axis=1, keepdims=True)))
    sig_gate = jax.nn.sigmoid(conv_gate.astype(jnp.float32))
    value_float = conv_value.astype(jnp.float32)
    gated_rows = lax.optimization_barrier((value_float * sig_gate).astype(jnp.bfloat16)).astype(jnp.float32)
    tap_reach = TAPS - 1
    padded_rows = jnp.pad(gated_rows, ((tap_reach, 0), (0, 0)))
    padded_grad = jnp.pad(height_grad, ((0, tap_reach), (0, 0)))
    tap_values = conv_taps.astype(jnp.float32)
    tap_list = []
    gated_grad = jnp.zeros_like(height_grad)
    for tap_index in range(TAPS):
        tap_list.append(lax.optimization_barrier(jnp.sum(height_grad * padded_rows[tap_index:tap_index + SEQ], axis=0)))
        begin = tap_reach - tap_index
        gated_grad = gated_grad + tap_values[tap_index] * padded_grad[begin:begin + SEQ]
    grad_taps = jnp.stack(tap_list)
    grad_value = (gated_grad * sig_gate).astype(jnp.bfloat16)
    grad_gate = (gated_grad * value_float * sig_gate * (1.0 - sig_gate)).astype(jnp.bfloat16)
    return (grad_value, grad_gate, grad_taps, grad_gain, grad_shift, grad_proj)
```

```python
import functools

import jax
import jax.numpy as jnp
from jax import lax
from jax.experimental import pallas as pl
from jax.experimental.pallas import tpu as pltpu
from jax.sharding import PartitionSpec as P

norm_eps = 1e-05
MESH = pl.DeviceIdType.MESH
F32 = jnp.float32
BF16 = jnp.bfloat16
LANES = 128


def bit(x, b):
    return lax.rem(x // (1 << b), 2)


def coordinate_bits(index, nbits):
    bits = [bit(index, b) for b in range(nbits)]
    if nbits >= 2:
        bits[nbits - 2] = lax.rem(bits[nbits - 2] + bits[nbits - 1], 2)
    return bits


def partner_of(me, b, nbits):
    def flip(x, c):
        return x + (1 << c) * (1 - 2 * bit(me, c))

    other = flip(me, b)
    if nbits >= 2 and b == nbits - 1:
        other = flip(other, b - 1)
    return other


def stage_orders(nbits, groups):
    body = list(range(max(nbits - 1, 1)))
    tail = list(range(len(body), nbits))
    return [body[g % len(body):] + body[: g % len(body)] + tail for g in range(groups)]


def kernel(
    dims,
    cv_hbm, cg_hbm, co_hbm, taps_ref, gain_ref, shift_ref, w_hbm, og_hbm,
    gv_hbm, gg_hbm, small_out, proj_out,
    cv, cg, co, w, og, ogt, active, normed, dsilu, scaled, hgx, gv, gg,
    st_a, st_b, st_c, st_d, acc, sendbuf, recvbuf, tapacc, rowacc, flat, parts, mine, whole,
    in_sem, out_sem, tp_send, tp_recv, halo_send, halo_recv,
    rs_send, rs_recv, a_send, a_recv, b_send, b_recv,
):
    n, nbits, groups, chan_total = dims
    rows, chan = co.shape
    width = og.shape[1]
    block = width // n
    gcols = chan // groups
    cblocks = chan // LANES
    ntaps = taps_ref.shape[1]
    reach = ntaps - 1
    halo = hgx.shape[1] - rows
    chunk = mine.shape[0]
    per = small_out.shape[0]
    me = lax.axis_index("sp")
    core = lax.axis_index("tp")
    other_core = 1 - core
    orders = stage_orders(nbits, groups)

    loads = [
        pltpu.make_async_copy(src, dst, in_sem.at[i])
        for i, (src, dst) in enumerate(
            ((co_hbm, co), (og_hbm, og), (w_hbm, w), (cg_hbm, cg), (cv_hbm, cv))
        )
    ]
    for copy in loads:
        copy.start()

    barrier = pltpu.get_barrier_semaphore()

    def greet(i, carry):
        pl.semaphore_signal(
            barrier, inc=1, device_id=(lax.rem(me + i, n), core), device_id_type=MESH
        )
        return carry

    lax.fori_loop(1, n, greet, 0)
    pl.semaphore_signal(barrier, inc=1, device_id=(me, other_core), device_id_type=MESH)

    lane_low = lax.broadcasted_iota(jnp.int32, (1, LANES), 1) < LANES // 2

    loads[0].wait()

    def stats(i, carry):
        at = pl.ds(pl.multiple_of(i * 64, 64), 64)
        h = co[at, :].astype(F32)
        mean = jnp.sum(h, axis=1, keepdims=True) / chan
        d = h - mean
        m2 = jnp.sum(d * d, axis=1, keepdims=True)
        st_a[at, :] = jnp.where(lane_low, mean, m2)
        return carry

    lax.fori_loop(0, rows // 64, stats, 0)
    pl.semaphore_wait(barrier, n)
    swap_a = pltpu.make_async_remote_copy(
        src_ref=st_a, dst_ref=st_b, send_sem=tp_send.at[0], recv_sem=tp_recv.at[0],
        device_id=(me, other_core), device_id_type=MESH,
    )
    swap_a.start()

    loads[1].wait()
    mybits = coordinate_bits(me, nbits)
    sub = LANES // block

    def transpose(c, carry):
        t = og[:, pl.ds(pl.multiple_of(c * LANES, LANES), LANES)].T
        for s in range(sub):
            rbits = coordinate_bits(c * sub + s, nbits)
            piece = t[s * block:(s + 1) * block, :]
            for g in range(groups):
                place = 0
                for k, b in enumerate(orders[g]):
                    place = place + lax.rem(rbits[b] + mybits[b], 2) * (1 << (nbits - 1 - k))
                ogt[g, place] = piece
        return carry

    lax.fori_loop(0, width // LANES, transpose, 0)

    swap_a.wait()
    half = 0.5 * chan

    def norm(i, carry):
        at = pl.ds(pl.multiple_of(i * 32, 32), 32)
        own, peer = st_a[at, :], st_b[at, :]
        mean_a, mean_b = own[:, :1], peer[:, :1]
        m2 = own[:, LANES // 2:LANES // 2 + 1] + peer[:, LANES // 2:LANES // 2 + 1]
        gap = mean_a - mean_b
        center = 0.5 * (mean_a + mean_b)
        inv = lax.rsqrt((m2 + gap * gap * half) / chan_total + norm_eps)
        z = (co[at, :].astype(F32) - center) * inv
        normed[at, :] = z
        x = z * gain_ref[...] + shift_ref[...]
        sig = jax.nn.sigmoid(x)
        active[at, :] = (x * sig).astype(BF16)
        dsilu[at, :] = sig * (1.0 + x * (1.0 - sig))
        st_d[at, :] = jnp.broadcast_to(inv, (32, LANES))
        return carry

    lax.fori_loop(0, rows // 32, norm, 0)

    def stage_copy(g, k):
        count = n >> (k + 1)
        off = n - (n >> k)
        return pltpu.make_async_remote_copy(
            src_ref=sendbuf.at[g, pl.ds(off, count)],
            dst_ref=recvbuf.at[g, pl.ds(off, count)],
            send_sem=rs_send.at[g, k],
            recv_sem=rs_recv.at[g, k],
            device_id=(partner_of(me, orders[g][k], nbits), core),
            device_id_type=MESH,
        )

    unit = max(1, n // 4)

    def product(g, start):
        lhs = ogt[g, pl.ds(start, unit)].reshape(unit * block, rows)
        out = jnp.dot(lhs, active[:, g * gcols:(g + 1) * gcols], preferred_element_type=F32)
        return out.reshape(unit, block, gcols)

    for g in range(groups):

        def far(i, carry, g=g):
            sendbuf[g, pl.ds(i * unit, unit)] = product(g, n // 2 + i * unit).astype(BF16)
            return carry

        lax.fori_loop(0, n // 2 // unit, far, 0)
        stage_copy(g, 0).start()
    for g in range(groups):

        def near(i, carry, g=g):
            acc[g, pl.ds(i * unit, unit)] = product(g, i * unit)
            return carry

        lax.fori_loop(0, n // 2 // unit, near, 0)

    def stage(k):
        count = n >> (k + 1)
        off = n - (n >> k)
        for g in range(groups):
            stage_copy(g, k).wait_recv()
            if k + 1 < nbits:
                keep = count // 2

                def pass_on(i, carry, g=g):
                    sendbuf[g, off + count + i] = (
                        acc[g, keep + i] + recvbuf[g, off + keep + i].astype(F32)
                    ).astype(BF16)
                    return carry

                lax.fori_loop(0, count - keep, pass_on, 0)
                stage_copy(g, k + 1).start()
            else:
                keep = count

            def take(i, carry, g=g):
                acc[g, i] = acc[g, i] + recvbuf[g, off + i].astype(F32)
                return carry

            lax.fori_loop(0, keep, take, 0)

    loads[2].wait()
    rowacc[...] = jnp.zeros_like(rowacc)

    def act(i, carry):
        at = pl.ds(pl.multiple_of(i * 128, 128), 128)
        scaled[at, :] = jnp.dot(og[at, :], w[...], preferred_element_type=F32)
        return carry

    lax.fori_loop(0, rows // 128, act, 0)

    def grads(i, carry):
        at = pl.ds(pl.multiple_of(i * 32, 32), 32)
        z = normed[at, :]
        ng = scaled[at, :] * dsilu[at, :]
        ngz = ng * z
        rowacc[0] = rowacc[0] + jnp.sum(ngz.reshape(4, 8, chan), axis=0)
        rowacc[1] = rowacc[1] + jnp.sum(ng.reshape(4, 8, chan), axis=0)
        gain = gain_ref[...]
        s = ng * gain
        scaled[at, :] = s
        total = jnp.sum(s, axis=1, keepdims=True)
        dot = jnp.sum(s * z, axis=1, keepdims=True)
        st_a[at, :] = jnp.where(lane_low, total, dot)
        return carry

    lax.fori_loop(0, rows // 32, grads, 0)
    swap_b = pltpu.make_async_remote_copy(
        src_ref=st_a, dst_ref=st_c, send_sem=tp_send.at[1], recv_sem=tp_recv.at[1],
        device_id=(me, other_core), device_id_type=MESH,
    )
    swap_b.start()
    tapacc[...] = jnp.zeros_like(tapacc)
    flat[...] = jnp.zeros_like(flat)
    swap_b.wait()

    def height(i, carry):
        at = pl.ds(pl.multiple_of(i * 32, 32), 32)
        sums = (st_a[at, :] + st_c[at, :]) / chan_total
        inv = st_d[at, :]
        total, dot = sums[:, :1], sums[:, LANES // 2:LANES // 2 + 1]
        hg = inv[:, :1] * (scaled[at, :] - total - normed[at, :] * dot)
        for c in range(cblocks):
            hgx[c, at, :] = hg[:, c * LANES:(c + 1) * LANES]
        return carry

    height(0, 0)
    halo_copy = pltpu.make_async_remote_copy(
        src_ref=hgx.at[:, pl.ds(0, halo)],
        dst_ref=hgx.at[:, pl.ds(rows, halo)],
        send_sem=halo_send, recv_sem=halo_recv,
        device_id=(lax.rem(me + n - 1, n), core), device_id_type=MESH,
    )

    @pl.when(me > 0)
    def _():
        halo_copy.start()

    lax.fori_loop(1, rows // 32, height, 0)

    @pl.when(me == n - 1)
    def _():
        hgx[:, rows:, :] = jnp.zeros((cblocks, halo, LANES), F32)

    loads[3].wait()
    loads[4].wait()
    stage(0)

    @pl.when(me < n - 1)
    def _():
        halo_copy.wait_recv()

    step = 64
    steps = rows // step

    def conv(i, carry):
        c = i // steps
        r = pl.multiple_of(lax.rem(i, steps) * step, step)
        at = pl.ds(r, step)
        cols = pl.ds(pl.multiple_of(c * LANES, LANES), LANES)
        sig = jax.nn.sigmoid(cg[at, cols].astype(F32))
        value = cv[at, cols].astype(F32)
        gated = (value * sig).astype(BF16).astype(F32)
        total = jnp.zeros((step, LANES), F32)
        for j in range(ntaps):
            h = hgx[c, pl.ds(r + reach - j, step), :]
            total = total + taps_ref[c, pl.ds(j, 1), :] * h
            tapacc[c, j] = tapacc[c, j] + jnp.sum((gated * h).reshape(step // 8, 8, LANES), axis=0)
        gv[at, cols] = (total * sig).astype(BF16)
        gg[at, cols] = (total * value * sig * (1.0 - sig)).astype(BF16)
        return carry

    cuts = [cblocks * steps * i // nbits for i in range(nbits + 1)]
    for k in range(nbits - 1):
        lax.fori_loop(cuts[k], cuts[k + 1], conv, 0)
        if k + 1 < nbits - 1:
            stage(k + 1)
    lax.fori_loop(cuts[nbits - 1], cuts[nbits], conv, 0)

    stores = [
        pltpu.make_async_copy(src, dst, out_sem.at[i])
        for i, (src, dst) in enumerate(((gv, gv_hbm), (gg, gg_hbm)))
    ]
    for copy in stores:
        copy.start()

    for c in range(cblocks):
        rowsum = jnp.sum(tapacc[c], axis=1)
        flat[c * per:c * per + ntaps, :] = rowsum
        for j in range(2):
            flat[c * per + ntaps + j:c * per + ntaps + j + 1, :] = jnp.sum(
                rowacc[j, :, c * LANES:(c + 1) * LANES], axis=0, keepdims=True
            )

    def spread(i):
        peer = lax.rem(me + i, n)
        return pltpu.make_async_remote_copy(
            src_ref=flat.at[pl.ds(pl.multiple_of(peer * chunk, chunk), chunk)],
            dst_ref=parts.at[me],
            send_sem=a_send.at[peer], recv_sem=a_recv.at[me],
            device_id=(peer, core), device_id_type=MESH,
        )

    def collect(i):
        peer = lax.rem(me + i, n)
        return pltpu.make_async_remote_copy(
            src_ref=mine,
            dst_ref=whole.at[pl.ds(pl.multiple_of(me * chunk, chunk), chunk)],
            send_sem=b_send.at[peer], recv_sem=b_recv.at[me],
            device_id=(peer, core), device_id_type=MESH,
        )

    def arrived_part(peer):
        return pltpu.make_async_remote_copy(
            src_ref=flat.at[pl.ds(pl.multiple_of(peer * chunk, chunk), chunk)],
            dst_ref=parts.at[peer],
            send_sem=a_send.at[peer], recv_sem=a_recv.at[peer],
            device_id=(peer, core), device_id_type=MESH,
        )

    def arrived_whole(peer):
        return pltpu.make_async_remote_copy(
            src_ref=mine,
            dst_ref=whole.at[pl.ds(pl.multiple_of(peer * chunk, chunk), chunk)],
            send_sem=b_send.at[peer], recv_sem=b_recv.at[peer],
            device_id=(peer, core), device_id_type=MESH,
        )

    def loop(body):
        def run(i, carry):
            body(i)
            return carry

        lax.fori_loop(1, n, run, 0)

    loop(lambda i: spread(i).start())
    mine[...] = flat[pl.ds(pl.multiple_of(me * chunk, chunk), chunk), :]

    stage(nbits - 1)
    for g in range(groups):
        proj_out[:, g * gcols:(g + 1) * gcols] = acc[g, 0]

    def add_part(i):
        peer = lax.rem(me + i, n)
        arrived_part(peer).wait_recv()
        mine[...] = mine[...] + parts[peer]

    loop(add_part)
    loop(lambda i: collect(i).start())
    whole[pl.ds(pl.multiple_of(me * chunk, chunk), chunk), :] = mine[...]
    loop(lambda i: arrived_whole(lax.rem(me + i, n)).wait_recv())
    for c in range(cblocks):
        small_out[:, c * LANES:(c + 1) * LANES] = whole[c * per:(c + 1) * per, :]

    loop(lambda i: arrived_part(lax.rem(me + i, n)).wait_send())
    loop(lambda i: arrived_whole(lax.rem(me + i, n)).wait_send())
    for g in range(groups):
        for k in range(nbits):
            stage_copy(g, k).wait_send()

    @pl.when(me > 0)
    def _():
        halo_copy.wait_send()

    for copy in stores:
        copy.wait()


def local(conv_value, conv_gate, conv_out, conv_taps, norm_gain, norm_shift, proj_weight, out_grad):
    rows, chan = conv_value.shape
    ntaps = conv_taps.shape[0]
    width = out_grad.shape[1]
    n = lax.axis_size("sp")
    nbits = n.bit_length() - 1
    assert 1 << nbits == n and lax.axis_size("tp") == 2
    groups = 3
    gcols = chan // groups
    block = width // n
    cblocks = chan // LANES
    halo = 32
    per = -(-(ntaps + 2) // 8) * 8
    chunk = -(-(-(-per * cblocks // n)) // 8) * 8
    dims = (n, nbits, groups, chan * 2)
    taps = conv_taps.astype(F32).reshape(ntaps, cblocks, LANES).transpose(1, 0, 2)
    hbm = pl.BlockSpec(memory_space=pl.ANY)
    vmem = pl.BlockSpec(memory_space=pltpu.VMEM)
    dma = pltpu.SemaphoreType.DMA
    grad_value, grad_gate, small, grad_proj = pl.pallas_call(
        functools.partial(kernel, dims),
        out_shape=(
            jax.ShapeDtypeStruct((rows, chan), BF16),
            jax.ShapeDtypeStruct((rows, chan), BF16),
            jax.ShapeDtypeStruct((per, chan), F32),
            jax.ShapeDtypeStruct((block, chan), F32),
        ),
        in_specs=[hbm, hbm, hbm, vmem, vmem, vmem, hbm, hbm],
        out_specs=(hbm, hbm, vmem, vmem),
        scratch_shapes=[
            pltpu.VMEM((rows, chan), BF16),
            pltpu.VMEM((rows, chan), BF16),
            pltpu.VMEM((rows, chan), BF16),
            pltpu.VMEM((width, chan), BF16),
            pltpu.VMEM((rows, width), BF16),
            pltpu.VMEM((groups, n, block, rows), BF16),
            pltpu.VMEM((rows, chan), BF16),
            pltpu.VMEM((rows, chan), F32),
            pltpu.VMEM((rows, chan), F32),
            pltpu.VMEM((rows, chan), F32),
            pltpu.VMEM((cblocks, rows + halo, LANES), F32),
            pltpu.VMEM((rows, chan), BF16),
            pltpu.VMEM((rows, chan), BF16),
            pltpu.VMEM((rows, LANES), F32),
            pltpu.VMEM((rows, LANES), F32),
            pltpu.VMEM((rows, LANES), F32),
            pltpu.VMEM((rows, LANES), F32),
            pltpu.VMEM((groups, n // 2, block, gcols), F32),
            pltpu.VMEM((groups, n, block, gcols), BF16),
            pltpu.VMEM((groups, n, block, gcols), BF16),
            pltpu.VMEM((cblocks, ntaps, 8, LANES), F32),
            pltpu.VMEM((2, 8, chan), F32),
            pltpu.VMEM((n * chunk, LANES), F32),
            pltpu.VMEM((n, chunk, LANES), F32),
            pltpu.VMEM((chunk, LANES), F32),
            pltpu.VMEM((n * chunk, LANES), F32),
            dma((5,)), dma((2,)),
            dma((2,)), dma((2,)),
            dma, dma,
            dma((groups, nbits)), dma((groups, nbits)),
            dma((n,)), dma((n,)),
            dma((n,)), dma((n,)),
        ],
        compiler_params=pltpu.CompilerParams(
            collective_id=0, has_side_effects=True, vmem_limit_bytes=60 * 1024 * 1024
        ),
    )(
        conv_value, conv_gate, conv_out, taps,
        norm_gain.reshape(1, chan), norm_shift.reshape(1, chan), proj_weight, out_grad,
    )
    return (grad_value, grad_gate, small[:ntaps], small[ntaps], small[ntaps + 1], grad_proj)


def solution(mesh):
    in_specs = (
        P("sp", "tp"),
        P("sp", "tp"),
        P("sp", "tp"),
        P(None, "tp"),
        P("tp"),
        P("tp"),
        P(None, "tp"),
        P("sp", None),
    )
    out_specs = (P("sp", "tp"), P("sp", "tp"), P(None, "tp"), P("tp"), P("tp"), P("sp", "tp"))
    return jax.shard_map(local, mesh=mesh, in_specs=in_specs, out_specs=out_specs, check_vma=False)
```

```python
import functools

import jax
import jax.numpy as jnp
from jax import lax
from jax.experimental import pallas as pl
from jax.experimental.pallas import tpu as pltpu
from jax.sharding import PartitionSpec as P

norm_eps = 1e-05
MESH = pl.DeviceIdType.MESH
F32 = jnp.float32
BF16 = jnp.bfloat16
LANES = 128


def repeat(start, stop, body, unroll):
    assert (stop - start) % unroll == 0

    def step(i, carry):
        for u in range(unroll):
            body(start + i * unroll + u, carry)
        return carry

    lax.fori_loop(0, (stop - start) // unroll, step, 0)


def bit(x, b):
    return lax.rem(x // (1 << b), 2)


def coordinate_bits(index, nbits):
    bits = [bit(index, b) for b in range(nbits)]
    if nbits >= 2:
        bits[nbits - 2] = lax.rem(bits[nbits - 2] + bits[nbits - 1], 2)
    return bits


def partner_of(me, b, nbits):
    def flip(x, c):
        return x + (1 << c) * (1 - 2 * bit(me, c))

    other = flip(me, b)
    if nbits >= 2 and b == nbits - 1:
        other = flip(other, b - 1)
    return other


def stage_orders(nbits, groups):
    body = list(range(max(nbits - 1, 1)))
    tail = list(range(len(body), nbits))
    return [body[g % len(body):] + body[: g % len(body)] + tail for g in range(groups)]


def kernel(
    dims,
    cv_hbm, cg_hbm, co_hbm, taps_ref, gain_ref, shift_ref, w_hbm, og_hbm,
    gv_hbm, gg_hbm, small_out, proj_out,
    cv, cg, co, w, og, ogt, active, normed, dsilu, scaled, hgx, gv, gg,
    st_a, st_b, st_d, pk_a, pk_b, pk_c, pk_d, tapf, acc, sendbuf, recvbuf, tapacc, rowacc, flat, parts, mine, whole,
    in_sem, out_sem, tp_send, tp_recv, halo_send, halo_recv,
    rs_send, rs_recv, a_send, a_recv, b_send, b_recv,
):
    n, nbits, groups, chan_total = dims
    rows, chan = co.shape
    width = og.shape[1]
    block = width // n
    gcols = chan // groups
    cblocks = chan // LANES
    ntaps = taps_ref.shape[0]
    reach = ntaps - 1
    halo = hgx.shape[1] - rows
    chunk = mine.shape[0]
    per = small_out.shape[0]
    me = lax.axis_index("sp")
    core = lax.axis_index("tp")
    other_core = 1 - core
    orders = stage_orders(nbits, groups)

    loads = [
        pltpu.make_async_copy(src, dst, in_sem.at[i])
        for i, (src, dst) in enumerate(
            ((co_hbm, co), (og_hbm, og), (w_hbm, w), (cg_hbm, cg), (cv_hbm, cv))
        )
    ]
    loads[0].start()

    barrier = pltpu.get_barrier_semaphore()

    def greet(i, carry):
        pl.semaphore_signal(
            barrier, inc=1, device_id=(lax.rem(me + i, n), core), device_id_type=MESH
        )
        return carry

    lax.fori_loop(1, n, greet, 0)
    pl.semaphore_signal(barrier, inc=1, device_id=(me, other_core), device_id_type=MESH)

    lane_low = lax.broadcasted_iota(jnp.int32, (1, LANES), 1) < LANES // 2

    gain = gain_ref[...].reshape(1, chan)
    shift = shift_ref[...].reshape(1, chan)
    nt = rows // LANES
    mid = LANES // 2

    def pack(dst):
        for t in range(nt):
            turned = st_a[t * LANES:(t + 1) * LANES, :].T
            dst[0, t:t + 1, :] = turned[:1, :]
            dst[1, t:t + 1, :] = turned[mid:mid + 1, :]

    def unpack(packed, dst):
        for t in range(nt):
            dst[t * LANES:(t + 1) * LANES, :] = jnp.broadcast_to(packed[t:t + 1, :], (LANES, LANES)).T

    def wide(x):
        return jnp.concatenate([x] * cblocks, axis=1)

    loads[0].wait()
    for copy in loads[1:]:
        copy.start()

    def stats(i, carry):
        at = pl.ds(pl.multiple_of(i * 64, 64), 64)
        h = co[at, :].astype(F32)
        mean = jnp.sum(h, axis=1, keepdims=True) / chan
        d = h - mean
        m2 = jnp.sum(d * d, axis=1, keepdims=True)
        st_a[at, :] = jnp.where(lane_low, mean, m2)
        return carry

    repeat(0, rows // 64, stats, 2)
    pack(pk_a)
    pl.semaphore_wait(barrier, n)
    swap_a = pltpu.make_async_remote_copy(
        src_ref=pk_a, dst_ref=pk_b, send_sem=tp_send.at[0], recv_sem=tp_recv.at[0],
        device_id=(me, other_core), device_id_type=MESH,
    )
    swap_a.start()

    loads[1].wait()
    mybits = coordinate_bits(me, nbits)
    sub = LANES // block

    def transpose(c, carry):
        t = og[:, pl.ds(pl.multiple_of(c * LANES, LANES), LANES)].T
        for s in range(sub):
            rbits = coordinate_bits(c * sub + s, nbits)
            piece = t[s * block:(s + 1) * block, :]
            for g in range(groups):
                place = 0
                for k, b in enumerate(orders[g]):
                    place = place + lax.rem(rbits[b] + mybits[b], 2) * (1 << (nbits - 1 - k))
                ogt[g, place] = piece
        return carry

    lax.fori_loop(0, width // LANES, transpose, 0)

    swap_a.wait()
    gap = pk_a[0] - pk_b[0]
    variance = (pk_a[1] + pk_b[1] + gap * gap * (0.5 * chan)) / chan_total
    unpack(0.5 * (pk_a[0] + pk_b[0]), st_b)
    unpack(lax.rsqrt(variance + norm_eps), st_d)

    def norm(i, carry):
        at = pl.ds(pl.multiple_of(i * 32, 32), 32)
        z = (co[at, :].astype(F32) - wide(st_b[at, :])) * wide(st_d[at, :])
        normed[at, :] = z
        x = z * gain + shift
        sig = jax.nn.sigmoid(x)
        active[at, :] = (x * sig).astype(BF16)
        dsilu[at, :] = sig * (1.0 + x * (1.0 - sig))
        return carry

    repeat(0, rows // 32, norm, 2)

    def stage_copy(g, k):
        count = n >> (k + 1)
        off = n - (n >> k)
        return pltpu.make_async_remote_copy(
            src_ref=sendbuf.at[g, pl.ds(off, count)],
            dst_ref=recvbuf.at[g, pl.ds(off, count)],
            send_sem=rs_send.at[g, k],
            recv_sem=rs_recv.at[g, k],
            device_id=(partner_of(me, orders[g][k], nbits), core),
            device_id_type=MESH,
        )

    unit = max(1, n // 4)

    def product(g, start):
        lhs = ogt[g, pl.ds(start, unit)].reshape(unit * block, rows)
        out = jnp.dot(lhs, active[:, g * gcols:(g + 1) * gcols], preferred_element_type=F32)
        return out.reshape(unit, block, gcols)

    for g in range(groups):

        def far(i, carry, g=g):
            sendbuf[g, pl.ds(i * unit, unit)] = product(g, n // 2 + i * unit).astype(BF16)
            return carry

        lax.fori_loop(0, n // 2 // unit, far, 0)
        stage_copy(g, 0).start()
    for g in range(groups):

        def near(i, carry, g=g):
            acc[g, pl.ds(i * unit, unit)] = product(g, i * unit)
            return carry

        lax.fori_loop(0, n // 2 // unit, near, 0)

    def stage(k):
        count = n >> (k + 1)
        off = n - (n >> k)
        for g in range(groups):
            stage_copy(g, k).wait_recv()
            if k + 1 < nbits:
                keep = count // 2

                def pass_on(i, carry, g=g):
                    sendbuf[g, off + count + i] = (
                        acc[g, keep + i] + recvbuf[g, off + keep + i].astype(F32)
                    ).astype(BF16)
                    return carry

                lax.fori_loop(0, count - keep, pass_on, 0)
                stage_copy(g, k + 1).start()
            else:
                keep = count

            def take(i, carry, g=g):
                acc[g, i] = acc[g, i] + recvbuf[g, off + i].astype(F32)
                return carry

            lax.fori_loop(0, keep, take, 0)

    loads[2].wait()
    rowacc[...] = jnp.zeros_like(rowacc)

    def act(i, carry):
        at = pl.ds(pl.multiple_of(i * 128, 128), 128)
        scaled[at, :] = jnp.dot(og[at, :], w[...], preferred_element_type=F32)
        return carry

    lax.fori_loop(0, rows // 128, act, 0)

    def grads(i, carry):
        at = pl.ds(pl.multiple_of(i * 32, 32), 32)
        z = normed[at, :]
        ng = scaled[at, :] * dsilu[at, :]
        ngz = ng * z
        rowacc[0] = rowacc[0] + jnp.sum(ngz.reshape(4, 8, chan), axis=0)
        rowacc[1] = rowacc[1] + jnp.sum(ng.reshape(4, 8, chan), axis=0)
        s = ng * gain
        scaled[at, :] = s
        total = jnp.sum(s, axis=1, keepdims=True)
        dot = jnp.sum(s * z, axis=1, keepdims=True)
        st_a[at, :] = jnp.where(lane_low, total, dot)
        return carry

    repeat(0, rows // 32, grads, 2)
    pack(pk_c)
    swap_b = pltpu.make_async_remote_copy(
        src_ref=pk_c, dst_ref=pk_d, send_sem=tp_send.at[1], recv_sem=tp_recv.at[1],
        device_id=(me, other_core), device_id_type=MESH,
    )
    swap_b.start()
    tapacc[...] = jnp.zeros_like(tapacc)
    for c in range(cblocks):
        tapf[c] = taps_ref[:, c * LANES:(c + 1) * LANES].astype(F32)
    flat[...] = jnp.zeros_like(flat)
    swap_b.wait()
    unpack((pk_c[0] + pk_d[0]) / chan_total, st_a)
    unpack((pk_c[1] + pk_d[1]) / chan_total, st_b)

    def height(i, carry):
        at = pl.ds(pl.multiple_of(i * 32, 32), 32)
        hg = wide(st_d[at, :]) * (
            scaled[at, :] - wide(st_a[at, :]) - normed[at, :] * wide(st_b[at, :])
        )
        for c in range(cblocks):
            hgx[c, at, :] = hg[:, c * LANES:(c + 1) * LANES]
        return carry

    height(0, 0)
    halo_copy = pltpu.make_async_remote_copy(
        src_ref=hgx.at[:, pl.ds(0, halo)],
        dst_ref=hgx.at[:, pl.ds(rows, halo)],
        send_sem=halo_send, recv_sem=halo_recv,
        device_id=(lax.rem(me + n - 1, n), core), device_id_type=MESH,
    )

    @pl.when(me > 0)
    def _():
        halo_copy.start()

    repeat(1, rows // 32, height, 3)

    @pl.when(me == n - 1)
    def _():
        hgx[:, rows:, :] = jnp.zeros((cblocks, halo, LANES), F32)

    loads[3].wait()
    loads[4].wait()
    stage(0)

    @pl.when(me < n - 1)
    def _():
        halo_copy.wait_recv()

    step = 64
    steps = rows // step

    def conv(i, carry):
        c = i // steps
        r = pl.multiple_of(lax.rem(i, steps) * step, step)
        at = pl.ds(r, step)
        cols = pl.ds(pl.multiple_of(c * LANES, LANES), LANES)
        sig = jax.nn.sigmoid(cg[at, cols].astype(F32))
        value = cv[at, cols].astype(F32)
        gated = (value * sig).astype(BF16).astype(F32)
        total = jnp.zeros((step, LANES), F32)
        for j in range(ntaps):
            h = hgx[c, pl.ds(r + reach - j, step), :]
            total = total + tapf[c, pl.ds(j, 1), :] * h
            tapacc[c, j] = tapacc[c, j] + jnp.sum((gated * h).reshape(step // 8, 8, LANES), axis=0)
        gv[at, cols] = (total * sig).astype(BF16)
        gg[at, cols] = (total * value * sig * (1.0 - sig)).astype(BF16)
        return carry

    cut = cblocks * steps * 3 // 4
    lax.fori_loop(0, cut, conv, 0)
    stage(1)
    lax.fori_loop(cut, cblocks * steps, conv, 0)

    stores = [
        pltpu.make_async_copy(src, dst, out_sem.at[i])
        for i, (src, dst) in enumerate(((gv, gv_hbm), (gg, gg_hbm)))
    ]
    for copy in stores:
        copy.start()

    for c in range(cblocks):
        rowsum = jnp.sum(tapacc[c], axis=1)
        flat[c * per:c * per + ntaps, :] = rowsum
        for j in range(2):
            flat[c * per + ntaps + j:c * per + ntaps + j + 1, :] = jnp.sum(
                rowacc[j, :, c * LANES:(c + 1) * LANES], axis=0, keepdims=True
            )

    def spread(i):
        peer = lax.rem(me + i, n)
        return pltpu.make_async_remote_copy(
            src_ref=flat.at[pl.ds(pl.multiple_of(peer * chunk, chunk), chunk)],
            dst_ref=parts.at[me],
            send_sem=a_send.at[peer], recv_sem=a_recv.at[me],
            device_id=(peer, core), device_id_type=MESH,
        )

    def collect(i):
        peer = lax.rem(me + i, n)
        return pltpu.make_async_remote_copy(
            src_ref=mine,
            dst_ref=whole.at[pl.ds(pl.multiple_of(me * chunk, chunk), chunk)],
            send_sem=b_send.at[peer], recv_sem=b_recv.at[me],
            device_id=(peer, core), device_id_type=MESH,
        )

    def arrived_part(peer):
        return pltpu.make_async_remote_copy(
            src_ref=flat.at[pl.ds(pl.multiple_of(peer * chunk, chunk), chunk)],
            dst_ref=parts.at[peer],
            send_sem=a_send.at[peer], recv_sem=a_recv.at[peer],
            device_id=(peer, core), device_id_type=MESH,
        )

    def arrived_whole(peer):
        return pltpu.make_async_remote_copy(
            src_ref=mine,
            dst_ref=whole.at[pl.ds(pl.multiple_of(peer * chunk, chunk), chunk)],
            send_sem=b_send.at[peer], recv_sem=b_recv.at[peer],
            device_id=(peer, core), device_id_type=MESH,
        )

    def loop(body):
        def run(i, carry):
            body(i)
            return carry

        lax.fori_loop(1, n, run, 0)

    loop(lambda i: spread(i).start())
    mine[...] = flat[pl.ds(pl.multiple_of(me * chunk, chunk), chunk), :]

    for k in range(2, nbits - 1):
        stage(k)

    def add_part(i):
        peer = lax.rem(me + i, n)
        arrived_part(peer).wait_recv()
        mine[...] = mine[...] + parts[peer]

    loop(add_part)
    loop(lambda i: collect(i).start())
    whole[pl.ds(pl.multiple_of(me * chunk, chunk), chunk), :] = mine[...]

    stage(nbits - 1)
    for g in range(groups):
        proj_out[:, g * gcols:(g + 1) * gcols] = acc[g, 0]
    loop(lambda i: arrived_whole(lax.rem(me + i, n)).wait_recv())
    for c in range(cblocks):
        small_out[:, c * LANES:(c + 1) * LANES] = whole[c * per:(c + 1) * per, :]

    loop(lambda i: arrived_part(lax.rem(me + i, n)).wait_send())
    loop(lambda i: arrived_whole(lax.rem(me + i, n)).wait_send())
    for g in range(groups):
        for k in range(nbits):
            stage_copy(g, k).wait_send()

    @pl.when(me > 0)
    def _():
        halo_copy.wait_send()

    for copy in stores:
        copy.wait()


def place(gv_in, gg_in, small, proj_in, gv_out, gg_out, taps, gain, shift, proj_out, gv, gg, proj, in_sem, out_sem):
    ins = [
        pltpu.make_async_copy(src, dst, in_sem.at[i])
        for i, (src, dst) in enumerate(((gv_in, gv), (gg_in, gg), (proj_in, proj)))
    ]
    outs = [
        pltpu.make_async_copy(src, dst, out_sem.at[i])
        for i, (src, dst) in enumerate(((gv, gv_out), (gg, gg_out), (proj, proj_out)))
    ]
    for copy in ins:
        copy.start()
    ntaps = taps.shape[0]
    taps[...] = small[:ntaps, :]
    gain[...] = small[ntaps, :]
    shift[...] = small[ntaps + 1, :]
    for came, goes in zip(ins, outs):
        came.wait()
        goes.start()
    for copy in outs:
        copy.wait()


def local(conv_value, conv_gate, conv_out, conv_taps, norm_gain, norm_shift, proj_weight, out_grad):
    rows, chan = conv_value.shape
    ntaps = conv_taps.shape[0]
    width = out_grad.shape[1]
    n = lax.axis_size("sp")
    nbits = n.bit_length() - 1
    assert 1 << nbits == n and lax.axis_size("tp") == 2
    groups = 3
    gcols = chan // groups
    block = width // n
    cblocks = chan // LANES
    halo = 32
    per = -(-(ntaps + 2) // 8) * 8
    chunk = -(-(-(-per * cblocks // n)) // 8) * 8
    dims = (n, nbits, groups, chan * 2)
    hbm = pl.BlockSpec(memory_space=pl.ANY)
    vmem = pl.BlockSpec(memory_space=pltpu.VMEM)
    dma = pltpu.SemaphoreType.DMA
    grad_value, grad_gate, small, grad_proj = pl.pallas_call(
        functools.partial(kernel, dims),
        out_shape=(
            jax.ShapeDtypeStruct((rows, chan), BF16),
            jax.ShapeDtypeStruct((rows, chan), BF16),
            jax.ShapeDtypeStruct((per, chan), F32),
            jax.ShapeDtypeStruct((block, chan), F32),
        ),
        in_specs=[hbm, hbm, hbm, vmem, vmem, vmem, hbm, hbm],
        out_specs=(hbm, hbm, vmem, vmem),
        scratch_shapes=[
            pltpu.VMEM((rows, chan), BF16),
            pltpu.VMEM((rows, chan), BF16),
            pltpu.VMEM((rows, chan), BF16),
            pltpu.VMEM((width, chan), BF16),
            pltpu.VMEM((rows, width), BF16),
            pltpu.VMEM((groups, n, block, rows), BF16),
            pltpu.VMEM((rows, chan), BF16),
            pltpu.VMEM((rows, chan), F32),
            pltpu.VMEM((rows, chan), F32),
            pltpu.VMEM((rows, chan), F32),
            pltpu.VMEM((cblocks, rows + halo, LANES), F32),
            pltpu.VMEM((rows, chan), BF16),
            pltpu.VMEM((rows, chan), BF16),
            pltpu.VMEM((rows, LANES), F32),
            pltpu.VMEM((rows, LANES), F32),
            pltpu.VMEM((rows, LANES), F32),
            *[pltpu.VMEM((2, rows // LANES, LANES), F32)] * 4,
            pltpu.VMEM((cblocks, ntaps, LANES), F32),
            pltpu.VMEM((groups, n // 2, block, gcols), F32),
            pltpu.VMEM((groups, n, block, gcols), BF16),
            pltpu.VMEM((groups, n, block, gcols), BF16),
            pltpu.VMEM((cblocks, ntaps, 8, LANES), F32),
            pltpu.VMEM((2, 8, chan), F32),
            pltpu.VMEM((n * chunk, LANES), F32),
            pltpu.VMEM((n, chunk, LANES), F32),
            pltpu.VMEM((chunk, LANES), F32),
            pltpu.VMEM((n * chunk, LANES), F32),
            dma((5,)), dma((2,)),
            dma((2,)), dma((2,)),
            dma, dma,
            dma((groups, nbits)), dma((groups, nbits)),
            dma((n,)), dma((n,)),
            dma((n,)), dma((n,)),
        ],
        compiler_params=pltpu.CompilerParams(
            collective_id=0, has_side_effects=True, vmem_limit_bytes=60 * 1024 * 1024
        ),
    )(
        conv_value, conv_gate, conv_out, conv_taps, norm_gain, norm_shift, proj_weight, out_grad,
    )
    return pl.pallas_call(
        place,
        out_shape=(
            jax.ShapeDtypeStruct((rows, chan), BF16),
            jax.ShapeDtypeStruct((rows, chan), BF16),
            jax.ShapeDtypeStruct((ntaps, chan), F32),
            jax.ShapeDtypeStruct((chan,), F32),
            jax.ShapeDtypeStruct((chan,), F32),
            jax.ShapeDtypeStruct((block, chan), F32),
        ),
        in_specs=[hbm, hbm, vmem, hbm],
        out_specs=(hbm, hbm, vmem, vmem, vmem, hbm),
        scratch_shapes=[
            pltpu.VMEM((rows, chan), BF16),
            pltpu.VMEM((rows, chan), BF16),
            pltpu.VMEM((block, chan), F32),
            dma((3,)), dma((3,)),
        ],
    )(grad_value, grad_gate, small, grad_proj)


def solution(mesh):
    in_specs = (
        P("sp", "tp"),
        P("sp", "tp"),
        P("sp", "tp"),
        P(None, "tp"),
        P("tp"),
        P("tp"),
        P(None, "tp"),
        P("sp", None),
    )
    out_specs = (P("sp", "tp"), P("sp", "tp"), P(None, "tp"), P("tp"), P("tp"), P("sp", "tp"))
    return jax.shard_map(local, mesh=mesh, in_specs=in_specs, out_specs=out_specs, check_vma=False)
```

```python
import functools

import jax
import jax.numpy as jnp
from jax import lax
from jax.experimental import pallas as pl
from jax.experimental.pallas import tpu as pltpu
from jax.sharding import PartitionSpec as P

norm_eps = 1e-05
MESH = pl.DeviceIdType.MESH
F32 = jnp.float32
BF16 = jnp.bfloat16
LANES = 128


def repeat(start, stop, body, unroll):
    assert (stop - start) % unroll == 0

    def step(i, carry):
        for u in range(unroll):
            body(start + i * unroll + u, carry)
        return carry

    lax.fori_loop(0, (stop - start) // unroll, step, 0)


def bit(x, b):
    return lax.rem(x // (1 << b), 2)


def coordinate_bits(index, nbits):
    bits = [bit(index, b) for b in range(nbits)]
    if nbits >= 2:
        bits[nbits - 2] = lax.rem(bits[nbits - 2] + bits[nbits - 1], 2)
    return bits


def partner_of(me, b, nbits):
    def flip(x, c):
        return x + (1 << c) * (1 - 2 * bit(me, c))

    other = flip(me, b)
    if nbits >= 2 and b == nbits - 1:
        other = flip(other, b - 1)
    return other


def stage_orders(nbits, groups):
    body = list(range(max(nbits - 1, 1)))
    tail = list(range(len(body), nbits))
    return [body[g % len(body):] + body[: g % len(body)] + tail for g in range(groups)]


def kernel(
    dims,
    cv_hbm, cg_hbm, co_hbm, taps_ref, gain_ref, shift_ref, w_hbm, og_hbm,
    gv_hbm, gg_hbm, small_out, proj_out,
    cv, cg, co, w, og, ogt, active, normed, dsilu, scaled, hgx, gv, gg,
    st_a, st_b, st_d, pk_a, pk_b, pk_c, pk_d, tapf, acc, sendbuf, recvbuf, tapacc, rowacc, flat, parts, mine, whole,
    in_sem, out_sem, tp_send, tp_recv, halo_send, halo_recv,
    rs_send, rs_recv, a_send, a_recv, b_send, b_recv,
):
    n, nbits, groups, chan_total = dims
    rows, chan = co.shape
    width = og.shape[1]
    block = width // n
    gcols = chan // groups
    cblocks = chan // LANES
    ntaps = taps_ref.shape[0]
    reach = ntaps - 1
    halo = hgx.shape[1] - rows
    chunk = mine.shape[0]
    per = small_out.shape[0]
    me = lax.axis_index("sp")
    core = lax.axis_index("tp")
    other_core = 1 - core
    orders = stage_orders(nbits, groups)

    loads = [
        pltpu.make_async_copy(src, dst, in_sem.at[i])
        for i, (src, dst) in enumerate(
            ((co_hbm, co), (og_hbm, og), (w_hbm, w), (cg_hbm, cg), (cv_hbm, cv))
        )
    ]
    loads[0].start()

    barrier = pltpu.get_barrier_semaphore()

    def greet(i, carry):
        pl.semaphore_signal(
            barrier, inc=1, device_id=(lax.rem(me + i, n), core), device_id_type=MESH
        )
        return carry

    lax.fori_loop(1, n, greet, 0)
    pl.semaphore_signal(barrier, inc=1, device_id=(me, other_core), device_id_type=MESH)

    lane_low = lax.broadcasted_iota(jnp.int32, (1, LANES), 1) < LANES // 2

    gain = gain_ref[...].reshape(1, chan)
    shift = shift_ref[...].reshape(1, chan)
    nt = rows // LANES
    mid = LANES // 2

    def pack(dst):
        for t in range(nt):
            turned = st_a[t * LANES:(t + 1) * LANES, :].T
            dst[0, t:t + 1, :] = turned[:1, :]
            dst[1, t:t + 1, :] = turned[mid:mid + 1, :]

    def unpack(packed, dst):
        for t in range(nt):
            dst[t * LANES:(t + 1) * LANES, :] = jnp.broadcast_to(packed[t:t + 1, :], (LANES, LANES)).T

    def wide(x):
        return jnp.concatenate([x] * cblocks, axis=1)

    loads[0].wait()
    for copy in loads[1:]:
        copy.start()

    def stats(i, carry):
        at = pl.ds(pl.multiple_of(i * 64, 64), 64)
        h = co[at, :].astype(F32)
        mean = jnp.sum(h, axis=1, keepdims=True) / chan
        d = h - mean
        m2 = jnp.sum(d * d, axis=1, keepdims=True)
        st_a[at, :] = jnp.where(lane_low, mean, m2)
        return carry

    repeat(0, rows // 64, stats, 2)
    pack(pk_a)
    pl.semaphore_wait(barrier, n)
    swap_a = pltpu.make_async_remote_copy(
        src_ref=pk_a, dst_ref=pk_b, send_sem=tp_send.at[0], recv_sem=tp_recv.at[0],
        device_id=(me, other_core), device_id_type=MESH,
    )
    swap_a.start()

    loads[1].wait()
    mybits = coordinate_bits(me, nbits)
    sub = LANES // block

    def transpose(c, carry):
        t = og[:, pl.ds(pl.multiple_of(c * LANES, LANES), LANES)].T
        for s in range(sub):
            rbits = coordinate_bits(c * sub + s, nbits)
            piece = t[s * block:(s + 1) * block, :]
            for g in range(groups):
                place = 0
                for k, b in enumerate(orders[g]):
                    place = place + lax.rem(rbits[b] + mybits[b], 2) * (1 << (nbits - 1 - k))
                ogt[g, place] = piece
        return carry

    lax.fori_loop(0, width // LANES, transpose, 0)

    swap_a.wait()
    gap = pk_a[0] - pk_b[0]
    variance = (pk_a[1] + pk_b[1] + gap * gap * (0.5 * chan)) / chan_total
    unpack(0.5 * (pk_a[0] + pk_b[0]), st_b)
    unpack(lax.rsqrt(variance + norm_eps), st_d)

    def norm(i, carry):
        at = pl.ds(pl.multiple_of(i * 32, 32), 32)
        z = (co[at, :].astype(F32) - wide(st_b[at, :])) * wide(st_d[at, :])
        normed[at, :] = z
        x = z * gain + shift
        sig = jax.nn.sigmoid(x)
        active[at, :] = (x * sig).astype(BF16)
        dsilu[at, :] = sig * (1.0 + x * (1.0 - sig))
        return carry

    repeat(0, rows // 32, norm, 2)

    def stage_copy(g, k):
        count = n >> (k + 1)
        off = n - (n >> k)
        return pltpu.make_async_remote_copy(
            src_ref=sendbuf.at[g, pl.ds(off, count)],
            dst_ref=recvbuf.at[g, pl.ds(off, count)],
            send_sem=rs_send.at[g, k],
            recv_sem=rs_recv.at[g, k],
            device_id=(partner_of(me, orders[g][k], nbits), core),
            device_id_type=MESH,
        )

    unit = max(1, n // 4)

    def product(g, start):
        lhs = ogt[g, pl.ds(start, unit)].reshape(unit * block, rows)
        out = jnp.dot(lhs, active[:, g * gcols:(g + 1) * gcols], preferred_element_type=F32)
        return out.reshape(unit, block, gcols)

    for g in range(groups):

        def far(i, carry, g=g):
            sendbuf[g, pl.ds(i * unit, unit)] = product(g, n // 2 + i * unit).astype(BF16)
            return carry

        lax.fori_loop(0, n // 2 // unit, far, 0)
        stage_copy(g, 0).start()
    def stage(k):
        count = n >> (k + 1)
        off = n - (n >> k)
        for g in range(groups):
            stage_copy(g, k).wait_recv()
            if k + 1 < nbits:
                keep = count // 2

                def pass_on(i, carry, g=g):
                    sendbuf[g, off + count + i] = (
                        acc[g, keep + i] + recvbuf[g, off + keep + i].astype(F32)
                    ).astype(BF16)
                    return carry

                lax.fori_loop(0, count - keep, pass_on, 0)
                stage_copy(g, k + 1).start()
            else:
                keep = count

            def take(i, carry, g=g):
                acc[g, i] = acc[g, i] + recvbuf[g, off + i].astype(F32)
                return carry

            lax.fori_loop(0, keep, take, 0)

    loads[2].wait()
    rowacc[...] = jnp.zeros_like(rowacc)

    def act(i, carry):
        at = pl.ds(pl.multiple_of(i * 128, 128), 128)
        scaled[at, :] = jnp.dot(og[at, :], w[...], preferred_element_type=F32)
        return carry

    lax.fori_loop(0, rows // 128, act, 0)

    def grads(i, carry):
        at = pl.ds(pl.multiple_of(i * 32, 32), 32)
        z = normed[at, :]
        ng = scaled[at, :] * dsilu[at, :]
        ngz = ng * z
        rowacc[0] = rowacc[0] + jnp.sum(ngz.reshape(4, 8, chan), axis=0)
        rowacc[1] = rowacc[1] + jnp.sum(ng.reshape(4, 8, chan), axis=0)
        s = ng * gain
        scaled[at, :] = s
        total = jnp.sum(s, axis=1, keepdims=True)
        dot = jnp.sum(s * z, axis=1, keepdims=True)
        st_a[at, :] = jnp.where(lane_low, total, dot)
        return carry

    repeat(0, rows // 32, grads, 2)
    pack(pk_c)
    swap_b = pltpu.make_async_remote_copy(
        src_ref=pk_c, dst_ref=pk_d, send_sem=tp_send.at[1], recv_sem=tp_recv.at[1],
        device_id=(me, other_core), device_id_type=MESH,
    )
    swap_b.start()
    tapacc[...] = jnp.zeros_like(tapacc)
    for c in range(cblocks):
        tapf[c] = taps_ref[:, c * LANES:(c + 1) * LANES].astype(F32)
    flat[...] = jnp.zeros_like(flat)
    for g in range(groups):

        def near(i, carry, g=g):
            acc[g, pl.ds(i * unit, unit)] = product(g, i * unit)
            return carry

        lax.fori_loop(0, n // 2 // unit, near, 0)

    swap_b.wait()
    unpack((pk_c[0] + pk_d[0]) / chan_total, st_a)
    unpack((pk_c[1] + pk_d[1]) / chan_total, st_b)

    def height(i, carry):
        at = pl.ds(pl.multiple_of(i * 32, 32), 32)
        hg = wide(st_d[at, :]) * (
            scaled[at, :] - wide(st_a[at, :]) - normed[at, :] * wide(st_b[at, :])
        )
        for c in range(cblocks):
            hgx[c, at, :] = hg[:, c * LANES:(c + 1) * LANES]
        return carry

    height(0, 0)
    halo_copy = pltpu.make_async_remote_copy(
        src_ref=hgx.at[:, pl.ds(0, halo)],
        dst_ref=hgx.at[:, pl.ds(rows, halo)],
        send_sem=halo_send, recv_sem=halo_recv,
        device_id=(lax.rem(me + n - 1, n), core), device_id_type=MESH,
    )

    @pl.when(me > 0)
    def _():
        halo_copy.start()

    repeat(1, rows // 32, height, 3)

    @pl.when(me == n - 1)
    def _():
        hgx[:, rows:, :] = jnp.zeros((cblocks, halo, LANES), F32)

    loads[3].wait()
    loads[4].wait()
    stage(0)

    @pl.when(me < n - 1)
    def _():
        halo_copy.wait_recv()

    step = 64
    steps = rows // step

    def conv(i, carry):
        c = i // steps
        r = pl.multiple_of(lax.rem(i, steps) * step, step)
        at = pl.ds(r, step)
        cols = pl.ds(pl.multiple_of(c * LANES, LANES), LANES)
        sig = jax.nn.sigmoid(cg[at, cols].astype(F32))
        value = cv[at, cols].astype(F32)
        gated = (value * sig).astype(BF16).astype(F32)
        total = jnp.zeros((step, LANES), F32)
        for j in range(ntaps):
            h = hgx[c, pl.ds(r + reach - j, step), :]
            total = total + tapf[c, pl.ds(j, 1), :] * h
            tapacc[c, j] = tapacc[c, j] + jnp.sum((gated * h).reshape(step // 8, 8, LANES), axis=0)
        gv[at, cols] = (total * sig).astype(BF16)
        gg[at, cols] = (total * value * sig * (1.0 - sig)).astype(BF16)
        return carry

    cut = cblocks * steps * 3 // 4
    lax.fori_loop(0, cut, conv, 0)
    stage(1)
    lax.fori_loop(cut, cblocks * steps, conv, 0)

    stores = [
        pltpu.make_async_copy(src, dst, out_sem.at[i])
        for i, (src, dst) in enumerate(((gv, gv_hbm), (gg, gg_hbm)))
    ]
    for copy in stores:
        copy.start()

    for c in range(cblocks):
        rowsum = jnp.sum(tapacc[c], axis=1)
        flat[c * per:c * per + ntaps, :] = rowsum
        for j in range(2):
            flat[c * per + ntaps + j:c * per + ntaps + j + 1, :] = jnp.sum(
                rowacc[j, :, c * LANES:(c + 1) * LANES], axis=0, keepdims=True
            )

    def spread(i):
        peer = lax.rem(me + i, n)
        return pltpu.make_async_remote_copy(
            src_ref=flat.at[pl.ds(pl.multiple_of(peer * chunk, chunk), chunk)],
            dst_ref=parts.at[me],
            send_sem=a_send.at[peer], recv_sem=a_recv.at[me],
            device_id=(peer, core), device_id_type=MESH,
        )

    def collect(i):
        peer = lax.rem(me + i, n)
        return pltpu.make_async_remote_copy(
            src_ref=mine,
            dst_ref=whole.at[pl.ds(pl.multiple_of(me * chunk, chunk), chunk)],
            send_sem=b_send.at[peer], recv_sem=b_recv.at[me],
            device_id=(peer, core), device_id_type=MESH,
        )

    def arrived_part(peer):
        return pltpu.make_async_remote_copy(
            src_ref=flat.at[pl.ds(pl.multiple_of(peer * chunk, chunk), chunk)],
            dst_ref=parts.at[peer],
            send_sem=a_send.at[peer], recv_sem=a_recv.at[peer],
            device_id=(peer, core), device_id_type=MESH,
        )

    def arrived_whole(peer):
        return pltpu.make_async_remote_copy(
            src_ref=mine,
            dst_ref=whole.at[pl.ds(pl.multiple_of(peer * chunk, chunk), chunk)],
            send_sem=b_send.at[peer], recv_sem=b_recv.at[peer],
            device_id=(peer, core), device_id_type=MESH,
        )

    def loop(body):
        def run(i, carry):
            body(i)
            return carry

        lax.fori_loop(1, n, run, 0)

    loop(lambda i: spread(i).start())
    mine[...] = flat[pl.ds(pl.multiple_of(me * chunk, chunk), chunk), :]

    for k in range(2, nbits - 1):
        stage(k)

    def add_part(i):
        peer = lax.rem(me + i, n)
        arrived_part(peer).wait_recv()
        mine[...] = mine[...] + parts[peer]

    loop(add_part)
    loop(lambda i: collect(i).start())
    whole[pl.ds(pl.multiple_of(me * chunk, chunk), chunk), :] = mine[...]

    stage(nbits - 1)
    for g in range(groups):
        proj_out[:, g * gcols:(g + 1) * gcols] = acc[g, 0]
    loop(lambda i: arrived_whole(lax.rem(me + i, n)).wait_recv())
    for c in range(cblocks):
        small_out[:, c * LANES:(c + 1) * LANES] = whole[c * per:(c + 1) * per, :]

    loop(lambda i: arrived_part(lax.rem(me + i, n)).wait_send())
    loop(lambda i: arrived_whole(lax.rem(me + i, n)).wait_send())
    for g in range(groups):
        for k in range(nbits):
            stage_copy(g, k).wait_send()

    @pl.when(me > 0)
    def _():
        halo_copy.wait_send()

    for copy in stores:
        copy.wait()


def place(gv_in, gg_in, small, proj_in, gv_out, gg_out, taps, gain, shift, proj_out, gv, gg, proj, in_sem, out_sem):
    ins = [
        pltpu.make_async_copy(src, dst, in_sem.at[i])
        for i, (src, dst) in enumerate(((gv_in, gv), (gg_in, gg), (proj_in, proj)))
    ]
    outs = [
        pltpu.make_async_copy(src, dst, out_sem.at[i])
        for i, (src, dst) in enumerate(((gv, gv_out), (gg, gg_out), (proj, proj_out)))
    ]
    for copy in ins:
        copy.start()
    ntaps = taps.shape[0]
    taps[...] = small[:ntaps, :]
    gain[...] = small[ntaps, :]
    shift[...] = small[ntaps + 1, :]
    for came, goes in zip(ins, outs):
        came.wait()
        goes.start()
    for copy in outs:
        copy.wait()


def local(conv_value, conv_gate, conv_out, conv_taps, norm_gain, norm_shift, proj_weight, out_grad):
    rows, chan = conv_value.shape
    ntaps = conv_taps.shape[0]
    width = out_grad.shape[1]
    n = lax.axis_size("sp")
    nbits = n.bit_length() - 1
    assert 1 << nbits == n and lax.axis_size("tp") == 2
    groups = 3
    gcols = chan // groups
    block = width // n
    cblocks = chan // LANES
    halo = 32
    per = -(-(ntaps + 2) // 8) * 8
    chunk = -(-(-(-per * cblocks // n)) // 8) * 8
    dims = (n, nbits, groups, chan * 2)
    hbm = pl.BlockSpec(memory_space=pl.ANY)
    vmem = pl.BlockSpec(memory_space=pltpu.VMEM)
    dma = pltpu.SemaphoreType.DMA
    grad_value, grad_gate, small, grad_proj = pl.pallas_call(
        functools.partial(kernel, dims),
        out_shape=(
            jax.ShapeDtypeStruct((rows, chan), BF16),
            jax.ShapeDtypeStruct((rows, chan), BF16),
            jax.ShapeDtypeStruct((per, chan), F32),
            jax.ShapeDtypeStruct((block, chan), F32),
        ),
        in_specs=[hbm, hbm, hbm, vmem, vmem, vmem, hbm, hbm],
        out_specs=(hbm, hbm, vmem, vmem),
        scratch_shapes=[
            pltpu.VMEM((rows, chan), BF16),
            pltpu.VMEM((rows, chan), BF16),
            pltpu.VMEM((rows, chan), BF16),
            pltpu.VMEM((width, chan), BF16),
            pltpu.VMEM((rows, width), BF16),
            pltpu.VMEM((groups, n, block, rows), BF16),
            pltpu.VMEM((rows, chan), BF16),
            pltpu.VMEM((rows, chan), F32),
            pltpu.VMEM((rows, chan), F32),
            pltpu.VMEM((rows, chan), F32),
            pltpu.VMEM((cblocks, rows + halo, LANES), F32),
            pltpu.VMEM((rows, chan), BF16),
            pltpu.VMEM((rows, chan), BF16),
            pltpu.VMEM((rows, LANES), F32),
            pltpu.VMEM((rows, LANES), F32),
            pltpu.VMEM((rows, LANES), F32),
            *[pltpu.VMEM((2, rows // LANES, LANES), F32)] * 4,
            pltpu.VMEM((cblocks, ntaps, LANES), F32),
            pltpu.VMEM((groups, n // 2, block, gcols), F32),
            pltpu.VMEM((groups, n, block, gcols), BF16),
            pltpu.VMEM((groups, n, block, gcols), BF16),
            pltpu.VMEM((cblocks, ntaps, 8, LANES), F32),
            pltpu.VMEM((2, 8, chan), F32),
            pltpu.VMEM((n * chunk, LANES), F32),
            pltpu.VMEM((n, chunk, LANES), F32),
            pltpu.VMEM((chunk, LANES), F32),
            pltpu.VMEM((n * chunk, LANES), F32),
            dma((5,)), dma((2,)),
            dma((2,)), dma((2,)),
            dma, dma,
            dma((groups, nbits)), dma((groups, nbits)),
            dma((n,)), dma((n,)),
            dma((n,)), dma((n,)),
        ],
        compiler_params=pltpu.CompilerParams(
            collective_id=0, has_side_effects=True, vmem_limit_bytes=60 * 1024 * 1024
        ),
    )(
        conv_value, conv_gate, conv_out, conv_taps, norm_gain, norm_shift, proj_weight, out_grad,
    )
    return pl.pallas_call(
        place,
        out_shape=(
            jax.ShapeDtypeStruct((rows, chan), BF16),
            jax.ShapeDtypeStruct((rows, chan), BF16),
            jax.ShapeDtypeStruct((ntaps, chan), F32),
            jax.ShapeDtypeStruct((chan,), F32),
            jax.ShapeDtypeStruct((chan,), F32),
            jax.ShapeDtypeStruct((block, chan), F32),
        ),
        in_specs=[hbm, hbm, vmem, hbm],
        out_specs=(hbm, hbm, vmem, vmem, vmem, hbm),
        scratch_shapes=[
            pltpu.VMEM((rows, chan), BF16),
            pltpu.VMEM((rows, chan), BF16),
            pltpu.VMEM((block, chan), F32),
            dma((3,)), dma((3,)),
        ],
    )(grad_value, grad_gate, small, grad_proj)


def solution(mesh):
    in_specs = (
        P("sp", "tp"),
        P("sp", "tp"),
        P("sp", "tp"),
        P(None, "tp"),
        P("tp"),
        P("tp"),
        P(None, "tp"),
        P("sp", None),
    )
    out_specs = (P("sp", "tp"), P("sp", "tp"), P(None, "tp"), P("tp"), P("tp"), P("sp", "tp"))
    return jax.shard_map(local, mesh=mesh, in_specs=in_specs, out_specs=out_specs, check_vma=False)
```
